32 devices in a mesh: gr: 2 (over x), fs: 8 (over z, y), tp: 2 (over core).
Axes of the slice: x: 2, y: 2, z: 4, core: 2. Of those that a mesh axis runs over, the one named last changes fastest.
Arguments:
- prompt_tokens: bfloat16 [4608, 2048], P(('gr', 'fs', 'tp')), may hold values from -6 to 6
- up_master: float32 [2048, 8192], P(('gr', 'fs'), 'tp'), may hold values from -0.125 to 0.125
- down_master: float32 [2048, 8192], P(('gr', 'fs'), 'tp'), may hold values from -0.0625 to 0.0625
- norm_gain: float32 [2048], P(('gr', 'fs')), may hold values from 0.1 to 1.9
Outputs:
- sampler_up: bfloat16 [2048, 8192], P(None, ('gr', 'tp'))
- sampler_down: bfloat16 [2048, 8192], P(None, ('gr', 'tp'))
- prompt_out: bfloat16 [4608, 2048], P(('gr', 'fs', 'tp'))
The draws below stay inside these ranges and needn't reach their ends.
All inputs are finite; a program needn't handle non-finite values.
Results may differ from the reference program's by a relative error of at most 0.009.
Values may be sent and summed in bfloat16 or wider, within the bound.
No kernel may reach another device: no remote copies, remote signals or barrier semaphores. Data moves between devices by JAX's collectives and lax.ppermute only.
A program may use at most 128 MiB of HBM per device.

```python
import jax
import jax.numpy as jnp
from jax import lax

D = 2048
FF = 8192
TOKENS = 4608
N_GR = 2
N_TP = 2


def steps_of(stream_key, dims, shards, low, high):
    level = 1.0
    for dim, parts in shards:
        draws = jax.random.uniform(jax.random.fold_in(jax.random.fold_in(stream_key, 6), dim), (parts,), jnp.float32, low / len(shards), high / len(shards))
        level = level * jnp.repeat(jnp.exp(draws), dims[dim] // parts).reshape((-1,) + (1,) * (len(dims) - 1 - dim))
    return level


def gaussian(own_key, shape, scale, reach, split=(), kind=jnp.bfloat16):
    drawn = jax.random.normal(own_key, shape, jnp.float32) * scale
    if len(split) > 0:
        drawn = steps_of(own_key, shape, split, -0.22, 0.18) * drawn
    return jnp.clip(drawn, min=-reach, max=reach).astype(kind)


def setup_inputs(seed: int = 0) -> dict:
    streams_of = jax.random.split(jax.random.key(seed), 5)
    prompt_tokens = gaussian(streams_of[0], (TOKENS, D), 1.0, 6.0, ((0, 32),))
    up_master = gaussian(streams_of[1], (D, FF), D ** -0.5, 0.125, ((0, 16), (1, 2)), jnp.float32)
    down_master = gaussian(streams_of[2], (D, FF), FF ** -0.5, 0.0625, ((0, 16), (1, 2)), jnp.float32)
    norm_gain = jnp.clip(1.0 + 0.18 * jax.random.normal(streams_of[3], (D,), jnp.float32), 0.1, 1.9)
    return {"prompt_tokens": prompt_tokens, "up_master": up_master, "down_master": down_master, "norm_gain": norm_gain}


def reference(prompt_tokens, up_master, down_master, norm_gain):
    sampler_up = (norm_gain[:, None] * up_master).astype(jnp.bfloat16)
    sampler_down = down_master.astype(jnp.bfloat16)
    values = prompt_tokens.astype(jnp.float32)
    center = lax.optimization_barrier(jnp.mean(values, axis=-1, keepdims=True))
    spread = lax.optimization_barrier(jnp.mean(jnp.square(values - center), axis=-1, keepdims=True))
    normed = ((values - center) * lax.rsqrt(spread + 1e-05)).astype(jnp.bfloat16)
    width = FF // (N_GR * N_TP)

    def block_step(total, index):
        start = (index * width).astype(jnp.int32)
        up_block = lax.dynamic_slice_in_dim(sampler_up, start, width, 1)
        down_block = lax.dynamic_slice_in_dim(sampler_down, start, width, 1)
        lifted = jax.nn.relu(jnp.dot(normed, up_block, preferred_element_type=jnp.float32))
        hidden = (lifted * lifted).astype(jnp.bfloat16)
        partial_value = lax.dot_general(hidden, down_block, (((1,), (1,)), ((), ())), preferred_element_type=jnp.float32)
        partial_value = lax.optimization_barrier(partial_value.astype(jnp.bfloat16)).astype(jnp.float32)
        return (total + partial_value, None)
    total, unused = lax.scan(block_step, jnp.zeros((TOKENS, D), jnp.float32), jnp.arange(N_GR * N_TP, dtype=jnp.int32))
    return (sampler_up, sampler_down, total.astype(jnp.bfloat16))
```

```python
import jax
import jax.numpy as jnp
from jax import lax
from jax.sharding import PartitionSpec as P


PAIR = 2
GROUP = ("gr", "tp")


def line_pairs(links):
    return [(p * PAIR + y, q * PAIR + y) for p, q in links for y in range(PAIR)]


def move(value, axes, links):
    return lax.ppermute(value, axes, links)


def grid_gather(chunk, length, pair_first):
    f = lax.axis_index("fs")
    z, y = f // PAIR, f % PAIR
    rows = chunk.shape[0]
    if length != 4:
        whole = lax.all_gather(chunk, "fs", axis=0, tiled=True)
        cut = [(i // PAIR, i % PAIR, whole[i * rows : (i + 1) * rows]) for i in range(length * PAIR)]
        middle = len(cut) // 2
        return cut[:middle], cut[middle:]

    def swap(value):
        return move(value, "fs", [(i, i ^ 1) for i in range(length * PAIR)])

    def line(first):
        got = move(first, "fs", line_pairs([(0, 1), (1, 0), (2, 3), (3, 2)]))
        near = lax.optimization_barrier(jnp.concatenate([first, got], axis=0))
        inner = move(near, "fs", line_pairs([(1, 2), (2, 1)]))
        outer = move(inner, "fs", line_pairs([(1, 0), (2, 3)]))
        return near, lax.optimization_barrier(jnp.where((z == 1) | (z == 2), inner, outer))

    mate = z ^ 1
    far_one, far_two = jnp.where(z < 2, 2, 1), jnp.where(z < 2, 3, 0)
    if pair_first:
        both = lax.optimization_barrier(jnp.concatenate([chunk, swap(chunk)], axis=0))
        near, far = line(both)
        places = [(z, y), (z, 1 - y), (mate, y), (mate, 1 - y)]
        far_places = [(far_one, y), (far_one, 1 - y), (far_two, y), (far_two, 1 - y)]
        return (
            [(*places[i], near[i * rows : (i + 1) * rows]) for i in range(4)],
            [(*far_places[i], far[i * rows : (i + 1) * rows]) for i in range(4)],
        )
    near, far = line(chunk)
    near_other, far_other = swap(near), swap(far)
    return (
        [(z, y, near[:rows]), (mate, y, near[rows:]), (z, 1 - y, near_other[:rows]), (mate, 1 - y, near_other[rows:])],
        [
            (far_one, y, far[:rows]),
            (far_two, y, far[rows:]),
            (far_one, 1 - y, far_other[:rows]),
            (far_two, 1 - y, far_other[rows:]),
        ],
    )


def body(prompt_tokens, up_master, down_master, norm_gain):
    shards = lax.axis_size("fs")
    length = shards // PAIR
    g = lax.axis_index("gr")
    t = lax.axis_index("tp")
    rows, half = up_master.shape
    width = half // lax.axis_size("tp")
    straight = t == g

    def piece(matrix, gain, u):
        cut = lax.dynamic_slice_in_dim(matrix, u * width, width, 1)
        if gain is not None:
            cut = gain[:, None] * cut
        return cut.astype(jnp.bfloat16)

    up_same, up_cross = piece(up_master, norm_gain, t), piece(up_master, norm_gain, 1 - t)
    down_same, down_cross = piece(down_master, None, t), piece(down_master, None, 1 - t)
    across = move(jnp.concatenate([up_cross, down_cross], axis=0), GROUP, [(0, 1), (3, 2)])
    up_a = lax.optimization_barrier(jnp.where(straight, up_same, across[:rows]))
    down_a = lax.optimization_barrier(jnp.where(straight, down_same, across[rows:]))

    def from_other_group(same, cross):
        near = move(same, GROUP, [(1, 3), (2, 0)])
        far = move(cross, GROUP, [(1, 2), (2, 1)])
        return lax.optimization_barrier(jnp.where(straight, near, far))

    up_b = from_other_group(up_same, up_cross)
    down_b = from_other_group(down_same, down_cross)

    values = prompt_tokens.astype(jnp.float32)
    center = jnp.mean(values, axis=-1, keepdims=True)
    variance = jnp.mean(jnp.square(values - center), axis=-1, keepdims=True)
    normed = ((values - center) * lax.rsqrt(variance + 1e-05)).astype(jnp.bfloat16)

    early = rows * 5 // 8 // 16 * 16

    def row_of(zz, yy):
        return (zz * PAIR + yy) * rows

    up_parts = [grid_gather(up_a, length, False), grid_gather(up_b, length, False)]
    down_parts = [
        (grid_gather(down_a[:-early], length, False), 0, 0),
        (grid_gather(down_b, length, False), 1, 0),
        (grid_gather(down_a[-early:], length, True), 0, rows - early),
    ]

    def base_of(cls):
        return (g if cls == 0 else 1 - g) * (shards * rows)

    total = rows * shards * lax.axis_size("gr")
    sampler_up = jnp.zeros((total, width), jnp.bfloat16)
    for cls, part in enumerate(up_parts):
        for zz, yy, block in part[0] + part[1]:
            sampler_up = lax.dynamic_update_slice_in_dim(sampler_up, block, base_of(cls) + row_of(zz, yy), 0)

    pairs = jnp.concatenate([normed, move(normed, GROUP, [(i, i ^ 1) for i in range(4)])], axis=0)
    tokens = jnp.concatenate([pairs, move(pairs, GROUP, [(i, i ^ 2) for i in range(4)])], axis=0)
    lifted = jax.nn.relu(jnp.dot(tokens, sampler_up, preferred_element_type=jnp.float32))
    hidden = (lifted * lifted).astype(jnp.bfloat16)
    count = normed.shape[0]

    def times_down(blocks):
        return lax.dot_general(
            hidden,
            jnp.concatenate(blocks, axis=0),
            (((1,), (1,)), ((), ())),
            preferred_element_type=jnp.float32,
        ).astype(jnp.bfloat16)

    sampler_down = jnp.zeros((total, width), jnp.bfloat16)
    prompt_out = jnp.zeros((count, total), jnp.bfloat16)
    for which in range(2):
        for part, cls, offset in down_parts:
            for zz, yy, block in part[which]:
                sampler_down = lax.dynamic_update_slice_in_dim(
                    sampler_down, block, base_of(cls) + row_of(zz, yy) + offset, 0
                )
        products = [
            (times_down([block for zz, yy, block in part[which]]), cls, offset, [(zz, yy) for zz, yy, b in part[which]])
            for part, cls, offset in down_parts
        ]
        slots = [(zz, yy) for zz, yy, block in down_parts[1][0][which]]
        own = []
        keep = rows - early
        order = [0, 2, 1, 3] if length == 4 else list(range(len(slots)))
        for i in range(len(slots)):
            j = order[i]
            own.append(products[0][0][:, i * keep : (i + 1) * keep])
            own.append(products[2][0][:, j * early : (j + 1) * early])
        class_a = jnp.concatenate(own, axis=1)
        class_b = products[1][0]
        partial = jnp.concatenate(
            [jnp.where(g == 0, class_a, class_b), jnp.where(g == 0, class_b, class_a)], axis=1
        )
        quarter = [partial[i * count : (i + 1) * count] for i in range(4)]
        got = move(jnp.concatenate([quarter[1], quarter[3]], axis=0), GROUP, [(i, i ^ 1) for i in range(4)]
        )
        mine = quarter[0].astype(jnp.float32) + got[:count].astype(jnp.float32)
        theirs = (quarter[2].astype(jnp.float32) + got[count:].astype(jnp.float32)).astype(jnp.bfloat16)
        rest = move(theirs, GROUP, [(i, i ^ 2) for i in range(4)])
        summed = (mine + rest.astype(jnp.float32)).astype(jnp.bfloat16)
        for side in range(2):
            for i, (zz, yy) in enumerate(slots):
                col = (side * len(slots) + i) * rows
                prompt_out = lax.dynamic_update_slice_in_dim(
                    prompt_out, summed[:, col : col + rows], side * shards * rows + row_of(zz, yy), 1
                )
    return (sampler_up, sampler_down, prompt_out)


def solution(mesh):
    placed = (
        P(("gr", "fs", "tp"), None),
        P(("gr", "fs"), "tp"),
        P(("gr", "fs"), "tp"),
        P(("gr", "fs")),
    )

    return jax.shard_map(
        body,
        mesh=mesh,
        in_specs=placed,
        out_specs=(P(None, ("gr", "tp")), P(None, ("gr", "tp")), P(("gr", "fs", "tp"), None)),
        check_vma=False,
    )
```
